32 devices in a mesh: dp: 4 (over y, x), kv: 4 (over z), tp: 2 (over core).
Axes of the slice: x: 2, y: 2, z: 4, core: 2. Of those that a mesh axis runs over, the one named last changes fastest.
Arguments:
- tokens: bfloat16 [256, 4096], P('dp', 'kv'), may hold values from -24 to 24
- state: float32 [256, 64, 64, 64], P(('dp', 'kv'), 'tp'), may hold values from -4 to 4
- w_query: bfloat16 [4096, 4096], P('kv', 'tp'), may hold values from -0.09375 to 0.09375
- w_forget: bfloat16 [4096, 4096], P('kv', 'tp'), may hold values from -0.09375 to 0.09375
- w_input: bfloat16 [4096, 4096], P('kv', 'tp'), may hold values from -0.09375 to 0.09375
- w_gate: bfloat16 [4096, 4096], P('kv', 'tp'), may hold values from -0.09375 to 0.09375
- lower_bound: float32 [4096], P('tp'), may hold values from 0 to 0.9
- head_gain: float32 [64], replicated, may hold values from 0.1 to 1.9
- w_out: bfloat16 [4096, 4096], P('tp', 'kv'), may hold values from -0.09375 to 0.09375
- gain_one: float32 [4096], P(('kv', 'tp')), may hold values from 0.1 to 1.9
- bias_one: float32 [4096], P(('kv', 'tp')), may hold values from -2 to 2
- w_up: bfloat16 [4096, 16384], P(None, ('kv', 'tp')), may hold values from -0.09375 to 0.09375
- w_down: bfloat16 [16384, 4096], P(('kv', 'tp')), may hold values from -0.0625 to 0.0625
- gain_two: float32 [4096], P(('kv', 'tp')), may hold values from 0.1 to 1.9
- bias_two: float32 [4096], P(('kv', 'tp')), may hold values from -2 to 2
Outputs:
- result: bfloat16 [256, 4096], P('dp', ('kv', 'tp'))
- new_state: float32 [256, 64, 64, 64], P(('dp', 'kv'), 'tp')
The draws below stay inside these ranges and needn't reach their ends.
All inputs are finite; a program needn't handle non-finite values.
Results may differ from the reference program's by a relative error of at most 0.014.
Values may be sent and summed in bfloat16 or wider, within the bound.
A program may use at most 128 MiB of HBM per device.

```python
import math
import jax
import jax.numpy as jnp
from jax import lax

D = 4096
HEADS = 64
DK = 64
FF = 16384
HW = 4096
BATCH = 256


def draw_tokens(key, part):
    key_base = jax.random.fold_in(key, 11)
    key_scale = jax.random.fold_in(key, 12)
    base = jnp.clip(jax.random.normal(key_base, (BATCH, D), jnp.float32), -8.0, 8.0)
    scales = jnp.exp(jax.random.uniform(key_scale, (16,), jnp.float32, math.log(0.3), math.log(3.0)))
    column_scale = jnp.repeat(scales, D // 16)
    return (base * column_scale[None, :]).astype(jnp.bfloat16)


def spiked(drawn, key, source, target, parts, factor):
    def block_of(dim):
        return (jnp.arange(drawn.shape[dim]) // (drawn.shape[dim] // parts)).reshape((-1,) + (1,) * (drawn.ndim - 1 - dim))

    one_side = jax.random.permutation(key, parts)[block_of(target)]
    far = (block_of(target) + parts // 2) % parts
    return jnp.where((block_of(source) == one_side) | (block_of(source) == far), factor * drawn, drawn)


def shard_levels(rng, shape, shards, smallest, high):
    def one(axis_at, shards_of):
        draws = jax.random.uniform(jax.random.fold_in(jax.random.fold_in(rng, 6), axis_at), (shards_of,), jnp.float32, smallest / len(shards), high / len(shards))
        return jnp.repeat(jnp.exp(draws), shape[axis_at] // shards_of).reshape((-1,) + (1,) * (len(shape) - axis_at - 1))

    loudness = one(*shards[0])
    for cut in shards[1:]:
        loudness = loudness * one(*cut)
    return loudness


def bell_draw(key, dims, scale, most, shards=(), held_as=jnp.bfloat16):
    entries = scale * jax.random.normal(key, dims, jnp.float32)
    if shards:
        entries = entries * shard_levels(key, dims, shards, -0.22, 0.18)
    return jnp.clip(entries, -most, most).astype(held_as)


def heavy_noise(rng, extent, deviation, reach, shards, heavy, kind=jnp.bfloat16):
    values = deviation * jax.random.normal(rng, extent, jnp.float32)
    if shards:
        values = values * shard_levels(rng, extent, shards, -0.22, 0.18)
    return jnp.clip(spiked(values, jax.random.fold_in(rng, 3), *heavy), -reach, reach).astype(kind)


def setup_inputs(seed: int = 0) -> dict:
    splits = jax.random.split(jax.random.key(seed), 16)
    return {
        "tokens": draw_tokens(jax.random.fold_in(splits[15], 71), 0),
        "state": bell_draw(splits[1], (BATCH, HEADS, DK, DK), 0.3, 4.0, ((0, 16), (1, 2)), jnp.float32),
        "w_query": bell_draw(splits[2], (D, HW), D ** -0.5, 0.09375, ((0, 4), (1, 2))),
        "w_forget": bell_draw(splits[3], (D, HW), D ** -0.5, 0.09375, ((0, 4), (1, 2))),
        "w_input": bell_draw(splits[4], (D, HW), D ** -0.5, 0.09375, ((0, 4), (1, 2))),
        "w_gate": bell_draw(splits[5], (D, HW), D ** -0.5, 0.09375, ((0, 4), (1, 2))),
        "lower_bound": jnp.clip(0.9 * jax.random.uniform(splits[6], (HW,), jnp.float32) ** shard_levels(splits[6], (HW,), ((0, 2),), -0.2, 0.2), 0.0, 0.9),
        "head_gain": jnp.clip(1.0 + 0.18 * jax.random.normal(splits[7], (DK,), jnp.float32), 0.1, 1.9),
        "w_out": bell_draw(splits[8], (HW, D), HW ** -0.5, 0.09375, ((0, 2), (1, 4))),
        "gain_one": jnp.clip(1.0 + 0.18 * jax.random.normal(splits[9], (D,), jnp.float32), 0.1, 1.9),
        "bias_one": bell_draw(splits[10], (D,), 0.3, 2.0, ((0, 8),), jnp.float32),
        "w_up": bell_draw(splits[11], (D, FF), D ** -0.5, 0.09375, ((1, 8),)),
        "w_down": heavy_noise(splits[12], (FF, D), FF ** -0.5, 0.0625, ((0, 8),), (0, 1, 8, 2.0)),
        "gain_two": jnp.clip(1.0 + 0.18 * jax.random.normal(splits[13], (D,), jnp.float32), 0.1, 1.9),
        "bias_two": bell_draw(splits[14], (D,), 0.3, 2.0, ((0, 8),), jnp.float32),
    }


epsilon = 0.1
residual_scale = 1.68

def layer_norm(values, gain, bias):
    center = lax.optimization_barrier(jnp.mean(values, axis=-1, keepdims=True))
    spread = lax.optimization_barrier(jnp.mean(jnp.square(values - center), axis=-1, keepdims=True))
    return (values - center) * lax.rsqrt(spread + epsilon) * gain + bias

def project(tokens, weight):
    rounded = jnp.dot(tokens, weight, preferred_element_type=jnp.float32).astype(jnp.bfloat16)
    rounded = lax.optimization_barrier(rounded)
    return rounded.astype(jnp.float32)

def reference(tokens, state, w_query, w_forget, w_input, w_gate, lower_bound, head_gain, w_out, gain_one, bias_one, w_up, w_down, gain_two, bias_two):
    batch = tokens.shape[0]
    shape = (batch, HEADS, DK)
    query_raw = project(tokens, w_query).reshape(shape)
    forget_raw = project(tokens, w_forget).reshape(shape)
    value_raw = project(tokens, w_input).reshape(shape)
    gate_raw = project(tokens, w_gate).reshape(shape)
    bound = lower_bound.reshape(HEADS, DK)
    forget = bound + (1.0 - bound) * jax.nn.sigmoid(forget_raw)
    keyvec = (1.0 - bound) * jax.nn.sigmoid(-forget_raw)
    query = jax.nn.silu(query_raw)
    new_state = forget[..., None] * state + keyvec[..., None] * value_raw[:, :, None, :]
    read = jnp.einsum('bhij,bhi->bhj', new_state, query, precision=lax.Precision.HIGHEST)
    read = read * lax.rsqrt(lax.optimization_barrier(jnp.mean(jnp.square(read), axis=-1, keepdims=True)) + epsilon)
    mixout = (read * head_gain * jax.nn.silu(gate_raw)).reshape(batch, HEADS * DK).astype(jnp.bfloat16)
    mixed = jnp.dot(mixout, w_out, preferred_element_type=jnp.float32)
    first = residual_scale * tokens.astype(jnp.float32) + mixed
    normed = layer_norm(first, gain_one, bias_one).astype(jnp.bfloat16)
    upper = jnp.dot(normed, w_up, preferred_element_type=jnp.float32)
    hidden = jnp.square(jax.nn.relu(upper)).astype(jnp.bfloat16)
    mlp = jnp.dot(hidden, w_down, preferred_element_type=jnp.float32)
    second = residual_scale * normed.astype(jnp.float32) + mlp
    result = layer_norm(second, gain_two, bias_two).astype(jnp.bfloat16)
    return (result, new_state)
```

```python
import functools

import jax
import jax.numpy as jnp
from jax import lax
from jax.experimental import pallas as pl
from jax.experimental.pallas import tpu as pltpu
from jax.sharding import PartitionSpec as P

epsilon = 0.1
residual_scale = 1.68
MESH = pl.DeviceIdType.MESH
VMEM_BYTES = 60 * 1024 * 1024


def shifted(index, by, count):
    return lax.rem(index + by, count)


def greet(peers):
    barrier = pltpu.get_barrier_semaphore()
    for peer in peers:
        pl.semaphore_signal(barrier, inc=1, device_id=peer, device_id_type=MESH)
    return lambda: pl.semaphore_wait(barrier, len(peers))


def send(source, target, send_sem, recv_sem, peer):
    copy = pltpu.make_async_remote_copy(
        src_ref=source,
        dst_ref=target,
        send_sem=send_sem,
        recv_sem=recv_sem,
        device_id=peer,
        device_id_type=MESH,
    )
    copy.start()
    return copy


def project_kernel(
    n, chunk, tokens, wq, wf, wi, wg, out, wbuf, whole, sent, got, load_sem, send_sem, recv_sem
):
    me = lax.axis_index("kv")
    weights = (wq, wf, wi, wg)
    per = wq.shape[1] // chunk
    chunks = len(weights) * per
    rows = out.shape[0]
    peers = [{"kv": shifted(me, o, n)} for o in range(1, n)]
    wait_barrier = greet(peers)
    loads = []
    for c in range(chunks):
        load = pltpu.make_async_copy(
            weights[c // per].at[:, pl.ds((c % per) * chunk, chunk)], wbuf.at[c], load_sem.at[c]
        )
        load.start()
        loads.append(load)
    copies = {}
    for c in range(chunks):
        loads[c].wait()
        value = jnp.dot(tokens[...], wbuf[c], preferred_element_type=jnp.float32)
        value = value.reshape(n, rows, chunk)
        whole[c] = value
        sent[c] = value.astype(jnp.bfloat16)
        if c == 0:
            wait_barrier()
        for o in range(1, n):
            copies[c, o] = send(
                sent.at[c, shifted(me, o, n)],
                got.at[c, o - 1],
                send_sem.at[c, o - 1],
                recv_sem.at[c, o - 1],
                peers[o - 1],
            )
    for c in range(chunks):
        total = whole[c, me]
        for o in range(1, n):
            copies[c, o].wait_recv()
            total = total + got[c, o - 1].astype(jnp.float32)
        out[:, c * chunk : (c + 1) * chunk] = total.astype(jnp.bfloat16)
    for copy in copies.values():
        copy.wait_send()


def project(tokens, weights, n):
    count = tokens.shape[0]
    rows = count // n
    depth, width = weights[0].shape
    chunk = min(width, 1024)
    chunks = len(weights) * (width // chunk)
    return pl.pallas_call(
        functools.partial(project_kernel, n, chunk),
        out_shape=jax.ShapeDtypeStruct((rows, len(weights) * width), jnp.bfloat16),
        in_specs=[pl.BlockSpec(memory_space=pltpu.VMEM)]
        + [pl.BlockSpec(memory_space=pl.ANY)] * len(weights),
        out_specs=pl.BlockSpec(memory_space=pltpu.VMEM),
        scratch_shapes=[
            pltpu.VMEM((chunks, depth, chunk), jnp.bfloat16),
            pltpu.VMEM((chunks, n, rows, chunk), jnp.float32),
            pltpu.VMEM((chunks, n, rows, chunk), jnp.bfloat16),
            pltpu.VMEM((chunks, n - 1, rows, chunk), jnp.bfloat16),
            pltpu.SemaphoreType.DMA((chunks,)),
            pltpu.SemaphoreType.DMA((chunks, n - 1)),
            pltpu.SemaphoreType.DMA((chunks, n - 1)),
        ],
        compiler_params=pltpu.CompilerParams(
            collective_id=0, has_side_effects=True, vmem_limit_bytes=VMEM_BYTES
        ),
        name="project",
    )(tokens, *weights)


def state_kernel(state, columns, bound, rows, gain, new_state, mixout, read):
    heads = state.shape[1]
    low = bound[...]
    query_raw = columns[0, 0].astype(jnp.float32)
    forget_raw = columns[0, 1].astype(jnp.float32)
    forget = low + (1.0 - low) * jax.nn.sigmoid(forget_raw)
    keyvec = (1.0 - low) * jax.nn.sigmoid(-forget_raw)
    query = query_raw * jax.nn.sigmoid(query_raw)
    value = rows[0, 0].astype(jnp.float32)
    gate = rows[0, 1].astype(jnp.float32)
    for h in range(heads):
        here = slice(h, h + 1)
        updated = forget[:, here] * state[0, h] + keyvec[:, here] * value[here, :]
        new_state[0, h] = updated
        read[here, :] = jnp.sum(updated * query[:, here], axis=0, keepdims=True)
    whole = read[...]
    scale = lax.rsqrt(jnp.mean(whole * whole, axis=1, keepdims=True) + epsilon)
    gated = whole * scale * gain[...] * (gate * jax.nn.sigmoid(gate))
    mixout[0] = gated.astype(jnp.bfloat16)


def update_state(state, columns, bound, rows, gain):
    count, heads, size, _ = state.shape
    return pl.pallas_call(
        state_kernel,
        grid=(count,),
        out_shape=(
            jax.ShapeDtypeStruct(state.shape, jnp.float32),
            jax.ShapeDtypeStruct((count, heads, size), jnp.bfloat16),
        ),
        in_specs=[
            pl.BlockSpec((1, heads, size, size), lambda b: (b, 0, 0, 0)),
            pl.BlockSpec((1, 2, size, heads), lambda b: (b, 0, 0, 0)),
            pl.BlockSpec((size, heads), lambda b: (0, 0)),
            pl.BlockSpec((1, 2, heads, size), lambda b: (b, 0, 0, 0)),
            pl.BlockSpec((1, size), lambda b: (0, 0)),
        ],
        out_specs=(
            pl.BlockSpec((1, heads, size, size), lambda b: (b, 0, 0, 0)),
            pl.BlockSpec((1, heads, size), lambda b: (b, 0, 0)),
        ),
        scratch_shapes=[pltpu.VMEM((heads, size), jnp.float32)],
        compiler_params=pltpu.CompilerParams(vmem_limit_bytes=VMEM_BYTES),
        name="state",
    )(state, columns, bound, rows, gain)


def to_lanes(column):
    count = column.shape[0]
    diagonal = lax.broadcasted_iota(jnp.int32, (count, count), 0) == lax.broadcasted_iota(
        jnp.int32, (count, count), 1
    )
    return jnp.sum(jnp.where(diagonal, column, 0.0), axis=0, keepdims=True)


def to_sublanes(row):
    count = row.shape[1]
    diagonal = lax.broadcasted_iota(jnp.int32, (count, count), 0) == lax.broadcasted_iota(
        jnp.int32, (count, count), 1
    )
    return jnp.sum(jnp.where(diagonal, row, 0.0), axis=1, keepdims=True)


def mix_kernel(
    n,
    t,
    mixout,
    tokens,
    one,
    two,
    w_out,
    w_up,
    w_down,
    out,
    out_buf,
    up_buf,
    down_buf,
    gathered,
    part,
    part_got,
    affine,
    firsts,
    normed,
    hidden,
    near_sent,
    near_got,
    kept,
    far_sent,
    far_got,
    stats,
    load_out,
    load_up,
    load_down,
    mix_send,
    mix_recv,
    part_send,
    part_recv,
    affine_send,
    affine_recv,
    first_send,
    first_recv,
    near_send,
    near_recv,
    far_send,
    far_recv,
    stats_send,
    stats_recv,
):
    kv, tp = lax.axis_index("kv"), lax.axis_index("tp")
    count, columns = out.shape
    rows = mixout.shape[0]
    group = n * t
    me = kv * t + tp
    width = group * columns
    offsets = [(o, u) for o in range(n) for u in range(t) if (o, u) != (0, 0)]

    def at(o, u):
        return {"kv": shifted(kv, o, n), "tp": shifted(tp, u, t)}

    def block(o, u):
        return shifted(kv, o, n) * t + shifted(tp, u, t)

    def columns_of(index):
        return pl.ds(pl.multiple_of(index * columns, columns), columns)

    wait_barrier = greet([at(o, u) for o, u in offsets])

    def load(source, target, sem):
        copy = pltpu.make_async_copy(source, target, sem)
        copy.start()
        return copy

    loads_out = [
        load(w_out.at[:, columns_of(shifted(tp, u, t))], out_buf.at[u], load_out.at[u])
        for u in range(t)
    ]
    up_chunks, _, up_width = up_buf.shape
    loads_up = [
        load(w_up.at[:, pl.ds(c * up_width, up_width)], up_buf.at[c], load_up.at[c])
        for c in range(up_chunks)
    ]
    steps = [*range(1, n), 0]
    loads_down = {
        (s, u): load(
            w_down.at[:, columns_of(block(steps[s], u))], down_buf.at[s, u], load_down.at[s, u]
        )
        for s in range(n)
        for u in range(t)
    }
    gathered[kv] = mixout[...]
    affine[me] = one[...]
    wait_barrier()
    pending = []

    mixes = [
        send(mixout, gathered.at[kv], mix_send.at[o], mix_recv.at[o], at(o, 0))
        for o in range(1, n)
    ]
    affines = [
        send(one, affine.at[me], affine_send.at[o, u], affine_recv.at[o, u], at(o, u))
        for o, u in offsets
    ]
    pending += mixes + affines
    for copy in mixes:
        copy.wait_recv()
    whole = gathered[...].reshape(count, gathered.shape[2])
    parts = []
    for u in [*range(1, t), 0]:
        loads_out[u].wait()
        product = jnp.dot(whole, out_buf[u], preferred_element_type=jnp.float32)
        if u:
            part[u - 1] = product
            parts.append(
                send(
                    part.at[u - 1],
                    part_got.at[u - 1],
                    part_send.at[u - 1],
                    part_recv.at[u - 1],
                    at(0, u),
                )
            )
    pending += parts
    own_tokens = tokens[:, columns_of(tp)].astype(jnp.float32)
    first = residual_scale * own_tokens + product
    for u in range(1, t):
        parts[u - 1].wait_recv()
        first = first + part_got[u - 1]
    firsts[me] = first.astype(jnp.bfloat16)

    def pass_on(index, o, u):
        where = at(o, u) if u == 0 else at(0, u)
        copy = send(
            firsts.at[index], firsts.at[index], first_send.at[o, u], first_recv.at[o, u], where
        )
        pending.append(copy)
        return copy

    passed = {}
    for o in range(1, n):
        passed[o, 0] = pass_on(me, o, 0)
    for u in range(1, t):
        passed[0, u] = pass_on(me, 0, u)
    for copy in affines:
        copy.wait_recv()
    for o in range(1, n):
        passed[o, 0].wait_recv()
        for u in range(1, t):
            passed[o, u] = pass_on(block(n - o, 0), o, u)
    for o in range(n):
        for u in range(1, t):
            passed[o, u].wait_recv()

    total = jnp.zeros((count, 1), jnp.float32)
    for g in range(group):
        total = total + jnp.sum(firsts[g].astype(jnp.float32), axis=1, keepdims=True)
    center = total / width
    spread = jnp.zeros((count, 1), jnp.float32)
    for g in range(group):
        away = firsts[g].astype(jnp.float32) - center
        spread = spread + jnp.sum(away * away, axis=1, keepdims=True)
    scale = lax.rsqrt(spread / width + epsilon)

    def finish(values, pair):
        return ((values.astype(jnp.float32) - center) * scale * pair[0:1] + pair[1:2]).astype(
            jnp.bfloat16
        )

    for g in range(group):
        normed[:, g * columns : (g + 1) * columns] = finish(firsts[g], affine[g])
    own_normed = finish(firsts[me], one[...])

    for c in range(up_chunks):
        loads_up[c].wait()
        upper = jnp.dot(normed[...], up_buf[c], preferred_element_type=jnp.float32)
        upper = jnp.maximum(upper, 0.0)
        hidden[:, c * up_width : (c + 1) * up_width] = (upper * upper).astype(jnp.bfloat16)

    near = {}
    far = {}

    def near_sum(s):
        value = kept[s]
        for u in range(1, t):
            near[s, u].wait_recv()
            value = value + near_got[s, u - 1].astype(jnp.float32)
        return value

    def far_out(s):
        far_sent[s] = near_sum(s).astype(jnp.bfloat16)
        far[s] = send(
            far_sent.at[s], far_got.at[s], far_send.at[s], far_recv.at[s], at(steps[s], 0)
        )

    for s in range(n):
        for u in [*range(1, t), 0]:
            loads_down[s, u].wait()
            product = jnp.dot(hidden[...], down_buf[s, u], preferred_element_type=jnp.float32)
            if u:
                near_sent[s, u - 1] = product.astype(jnp.bfloat16)
                near[s, u] = send(
                    near_sent.at[s, u - 1],
                    near_got.at[s, u - 1],
                    near_send.at[s, u - 1],
                    near_recv.at[s, u - 1],
                    at(0, u),
                )
            else:
                kept[s] = product
        if s:
            far_out(s - 1)
    second = residual_scale * own_normed.astype(jnp.float32) + near_sum(n - 1)
    for s in range(n - 1):
        far[s].wait_recv()
        second = second + far_got[s].astype(jnp.float32)
    pending += list(near.values()) + list(far.values())

    sums = jnp.concatenate(
        [
            to_lanes(jnp.sum(second, axis=1, keepdims=True)),
            to_lanes(jnp.sum(second * second, axis=1, keepdims=True)),
        ],
        axis=0,
    )
    stats[0, 0:2] = sums
    tallies = []
    for i, (o, u) in enumerate(offsets):
        tallies.append(
            send(stats.at[0], stats.at[i + 1], stats_send.at[i], stats_recv.at[i], at(o, u))
        )
    pending += tallies
    for i, copy in enumerate(tallies):
        copy.wait_recv()
        sums = sums + stats[i + 1, 0:2]
    center_two = to_sublanes(sums[0:1]) / width
    spread_two = to_sublanes(sums[1:2]) / width - center_two * center_two
    result = (second - center_two) * lax.rsqrt(spread_two + epsilon) * two[0:1] + two[1:2]
    out[...] = result.astype(jnp.bfloat16)
    for copy in pending:
        copy.wait_send()


def mix(mixout, tokens, one, two, w_out, w_up, w_down, n, t):
    count = tokens.shape[0]
    rows, heads_width = mixout.shape
    columns = one.shape[1]
    depth, units = w_up.shape
    group = n * t
    up_width = min(units, 512)
    dma = pltpu.SemaphoreType.DMA
    vmem = pltpu.VMEM
    few, many = jnp.bfloat16, jnp.float32
    return pl.pallas_call(
        functools.partial(mix_kernel, n, t),
        out_shape=jax.ShapeDtypeStruct((count, columns), few),
        in_specs=[pl.BlockSpec(memory_space=pltpu.VMEM)] * 4
        + [pl.BlockSpec(memory_space=pl.ANY)] * 3,
        out_specs=pl.BlockSpec(memory_space=pltpu.VMEM),
        scratch_shapes=[
            vmem((t, heads_width, columns), few),
            vmem((units // up_width, depth, up_width), few),
            vmem((n, t, units, columns), few),
            vmem((n, rows, heads_width), few),
            vmem((t - 1, count, columns), many),
            vmem((t - 1, count, columns), many),
            vmem((group, 2, columns), many),
            vmem((group, count, columns), few),
            vmem((count, depth), few),
            vmem((count, units), few),
            vmem((n, t - 1, count, columns), few),
            vmem((n, t - 1, count, columns), few),
            vmem((n, count, columns), many),
            vmem((n, count, columns), few),
            vmem((n, count, columns), few),
            vmem((group, 8, count), many),
            dma((t,)),
            dma((units // up_width,)),
            dma((n, t)),
            dma((n,)),
            dma((n,)),
            dma((t,)),
            dma((t,)),
            dma((n, t)),
            dma((n, t)),
            dma((n, t)),
            dma((n, t)),
            dma((n, t)),
            dma((n, t)),
            dma((n,)),
            dma((n,)),
            dma((group,)),
            dma((group,)),
        ],
        compiler_params=pltpu.CompilerParams(
            collective_id=1, has_side_effects=True, vmem_limit_bytes=VMEM_BYTES
        ),
        name="mix",
    )(mixout, tokens, one, two, w_out, w_up, w_down)


def per_device(
    tokens,
    state,
    w_query,
    w_forget,
    w_input,
    w_gate,
    lower_bound,
    head_gain,
    w_out,
    gain_one,
    bias_one,
    w_up,
    w_down,
    gain_two,
    bias_two,
):
    n, t = lax.axis_size("kv"), lax.axis_size("tp")
    rows = tokens.shape[0] // n
    size = head_gain.shape[0]
    heads = w_query.shape[1] // size
    projected = project(tokens, (w_query, w_forget, w_input, w_gate), n)
    projected = projected.reshape(rows, 4, heads, size)
    new_state, mixout = update_state(
        state,
        projected[:, :2].swapaxes(2, 3),
        lower_bound.reshape(heads, size).swapaxes(0, 1),
        projected[:, 2:],
        head_gain[None, :],
    )
    result = mix(
        mixout.reshape(rows, heads * size),
        tokens,
        jnp.stack([gain_one, bias_one]),
        jnp.stack([gain_two, bias_two]),
        w_out,
        w_up,
        w_down,
        n,
        t,
    )
    return (result, new_state)


def solution(mesh):
    placed = (
        P("dp", "kv"),
        P(("dp", "kv"), "tp", None, None),
        P("kv", "tp"),
        P("kv", "tp"),
        P("kv", "tp"),
        P("kv", "tp"),
        P("tp"),
        P(),
        P("tp", "kv"),
        P(("kv", "tp")),
        P(("kv", "tp")),
        P(None, ("kv", "tp")),
        P(("kv", "tp"), None),
        P(("kv", "tp")),
        P(("kv", "tp")),
    )
    return jax.shard_map(
        per_device,
        mesh=mesh,
        in_specs=placed,
        out_specs=(P("dp", ("kv", "tp")), P(("dp", "kv"), "tp", None, None)),
        check_vma=False,
    )
```

```python
import functools

import jax
import jax.numpy as jnp
import numpy as np
from jax import lax
from jax.experimental import pallas as pl
from jax.experimental.pallas import tpu as pltpu
from jax.sharding import PartitionSpec as P

epsilon = 0.1
residual_scale = 1.68
MESH = pl.DeviceIdType.MESH
VMEM_BYTES = 60 * 1024 * 1024


def shifted(index, by, count):
    return lax.rem(index + by, count)


def greet(peers):
    barrier = pltpu.get_barrier_semaphore()
    for peer in peers:
        pl.semaphore_signal(barrier, inc=1, device_id=peer, device_id_type=MESH)
    return lambda: pl.semaphore_wait(barrier, len(peers))


def send(source, target, send_sem, recv_sem, peer):
    copy = pltpu.make_async_remote_copy(
        src_ref=source,
        dst_ref=target,
        send_sem=send_sem,
        recv_sem=recv_sem,
        device_id=peer,
        device_id_type=MESH,
    )
    copy.start()
    return copy


def project_kernel(
    n,
    chunk,
    size,
    tokens,
    bound,
    gain,
    wq,
    wf,
    wi,
    wg,
    columns,
    lines,
    wbuf,
    whole,
    sent,
    got,
    load_sem,
    send_sem,
    recv_sem,
):
    me = lax.axis_index("kv")
    weights = (wq, wf, wi, wg)
    per = wq.shape[1] // chunk
    chunks = len(weights) * per
    rows = lines.shape[1]
    peers = [{"kv": shifted(me, o, n)} for o in range(1, n)]
    wait_barrier = greet(peers)
    order = [w * per + j for j in range(per) for w in range(len(weights))]
    loads = {}
    for c in order:
        loads[c] = pltpu.make_async_copy(
            weights[c // per].at[:, pl.ds((c % per) * chunk, chunk)], wbuf.at[c], load_sem.at[c]
        )
        loads[c].start()
    copies = {}
    for c in order:
        loads[c].wait()
        value = jnp.dot(tokens[...], wbuf[c], preferred_element_type=jnp.float32)
        value = value.reshape(n, rows, chunk)
        whole[c] = value
        sent[c] = value.astype(jnp.bfloat16)
        if c == order[0]:
            wait_barrier()
        for o in range(1, n):
            copies[c, o] = send(
                sent.at[c, shifted(me, o, n)],
                got.at[c, o - 1],
                send_sem.at[c, o - 1],
                recv_sem.at[c, o - 1],
                peers[o - 1],
            )

    def summed(c):
        total = whole[c, me]
        for o in range(1, n):
            copies[c, o].wait_recv()
            total = total + got[c, o - 1].astype(jnp.float32)
        return total.astype(jnp.bfloat16).astype(jnp.float32)

    heads = chunk // size
    for j in range(per):
        here = slice(j * chunk, (j + 1) * chunk)
        query_raw, forget_raw, value, gate = (summed(w * per + j) for w in range(len(weights)))
        low = bound[:, here]
        forget = low + (1.0 - low) * jax.nn.sigmoid(forget_raw)
        keyvec = (1.0 - low) * jax.nn.sigmoid(-forget_raw)
        high = keyvec.astype(jnp.bfloat16).astype(jnp.float32)
        stacked = jnp.concatenate([forget, high, keyvec - high], axis=0)
        columns[j * heads : (j + 1) * heads] = stacked.T.reshape(heads, size, 3 * rows)
        lines[0, :, here] = query_raw * jax.nn.sigmoid(query_raw)
        lines[1, :, here] = value
        lines[2, :, here] = gain[:, here] * gate * jax.nn.sigmoid(gate)
    for copy in copies.values():
        copy.wait_send()


def project(tokens, bound, gain, weights, n, size):
    count = tokens.shape[0]
    rows = count // n
    depth, width = weights[0].shape
    chunk = min(width, 1024)
    chunks = len(weights) * (width // chunk)
    vmem = pl.BlockSpec(memory_space=pltpu.VMEM)
    return pl.pallas_call(
        functools.partial(project_kernel, n, chunk, size),
        out_shape=(
            jax.ShapeDtypeStruct((width // size, size, 3 * rows), jnp.float32),
            jax.ShapeDtypeStruct((3, rows, width), jnp.float32),
        ),
        in_specs=[vmem] * 3 + [pl.BlockSpec(memory_space=pl.ANY)] * len(weights),
        out_specs=(vmem, vmem),
        scratch_shapes=[
            pltpu.VMEM((chunks, depth, chunk), jnp.bfloat16),
            pltpu.VMEM((chunks, n, rows, chunk), jnp.float32),
            pltpu.VMEM((chunks, n, rows, chunk), jnp.bfloat16),
            pltpu.VMEM((chunks, n - 1, rows, chunk), jnp.bfloat16),
            pltpu.SemaphoreType.DMA((chunks,)),
            pltpu.SemaphoreType.DMA((chunks, n - 1)),
            pltpu.SemaphoreType.DMA((chunks, n - 1)),
        ],
        compiler_params=pltpu.CompilerParams(
            collective_id=0, has_side_effects=True, vmem_limit_bytes=VMEM_BYTES
        ),
        name="project",
    )(tokens, bound, gain, *weights)


def split(values):
    high = values.astype(jnp.bfloat16)
    return high, (values - high.astype(jnp.float32)).astype(jnp.bfloat16)


def state_kernel(state, columns, lines, pick, new_state, mixout):
    count, heads, size, _ = state.shape
    row = lax.broadcasted_iota(jnp.int32, (count, size), 0)
    gated = []
    for h in range(heads):

        def turned(values):
            return pltpu.roll(values, (heads - h) * size, 1) if h else values

        query, query_rest = split(turned(lines[0])[:, :size])
        query = jnp.concatenate([query, query, query_rest], axis=1)
        value = turned(lines[1]).astype(jnp.bfloat16)
        value = jnp.concatenate([value] * 3, axis=0)
        column = columns[h]
        factors = column.astype(jnp.bfloat16)
        read = jnp.zeros((count, size), jnp.float32)
        for pair in range(0, count, 2):
            spread = jnp.concatenate([value * pick[pair], value * pick[pair + 1]], axis=1)
            outer = jnp.dot(factors, spread, preferred_element_type=jnp.float32)
            lanes = outer.shape[1] // 2
            for i in range(2):
                b = pair + i
                added = outer[:, i * lanes : i * lanes + size]
                updated = column[:, b : b + 1] * state[b, h] + added
                new_state[b, h] = updated
                high, rest = split(updated)
                product = jnp.dot(
                    query,
                    jnp.concatenate([high, rest, high], axis=0),
                    preferred_element_type=jnp.float32,
                )
                read = jnp.where(row == b, product, read)
        scale = lax.rsqrt(jnp.mean(read * read, axis=1, keepdims=True) + epsilon)
        gated.append(read * scale * turned(lines[2])[:, :size])
    mixout[...] = jnp.concatenate(gated, axis=1).astype(jnp.bfloat16)


def update_state(state, columns, lines):
    count, heads, size, _ = state.shape
    lanes = 128
    some = lanes // size
    index = np.arange(3 * count)
    pick = (index % count == np.arange(count)[:, None]) & (index >= count)
    pick = jnp.asarray(pick[:, :, None] & (np.arange(lanes) < size), jnp.bfloat16)
    return pl.pallas_call(
        state_kernel,
        grid=(heads // some,),
        out_shape=(
            jax.ShapeDtypeStruct(state.shape, jnp.float32),
            jax.ShapeDtypeStruct((count, heads * size), jnp.bfloat16),
        ),
        in_specs=[
            pl.BlockSpec((count, some, size, size), lambda h: (0, h, 0, 0)),
            pl.BlockSpec((some, size, 3 * count), lambda h: (h, 0, 0)),
            pl.BlockSpec((3, count, lanes), lambda h: (0, 0, h)),
            pl.BlockSpec((count, 3 * count, lanes), lambda h: (0, 0, 0)),
        ],
        out_specs=(
            pl.BlockSpec((count, some, size, size), lambda h: (0, h, 0, 0)),
            pl.BlockSpec((count, lanes), lambda h: (0, h)),
        ),
        compiler_params=pltpu.CompilerParams(vmem_limit_bytes=VMEM_BYTES),
        name="state",
    )(state, columns, lines, pick)


def to_lanes(column):
    count = column.shape[0]
    diagonal = lax.broadcasted_iota(jnp.int32, (count, count), 0) == lax.broadcasted_iota(
        jnp.int32, (count, count), 1
    )
    return jnp.sum(jnp.where(diagonal, column, 0.0), axis=0, keepdims=True)


def to_sublanes(row):
    count = row.shape[1]
    diagonal = lax.broadcasted_iota(jnp.int32, (count, count), 0) == lax.broadcasted_iota(
        jnp.int32, (count, count), 1
    )
    return jnp.sum(jnp.where(diagonal, row, 0.0), axis=1, keepdims=True)


def mix_kernel(
    n,
    t,
    mixout,
    tokens,
    gain_one,
    bias_one,
    gain_two,
    bias_two,
    w_out,
    w_up,
    w_down,
    out,
    out_buf,
    up_buf,
    down_buf,
    gathered,
    part,
    part_got,
    affine,
    firsts,
    normed,
    hidden,
    near_sent,
    near_got,
    kept,
    far_sent,
    far_got,
    stats,
    load_out,
    load_up,
    load_down,
    mix_send,
    mix_recv,
    part_send,
    part_recv,
    affine_send,
    affine_recv,
    first_send,
    first_recv,
    near_send,
    near_recv,
    far_send,
    far_recv,
    stats_send,
    stats_recv,
):
    kv, tp = lax.axis_index("kv"), lax.axis_index("tp")
    count, columns = out.shape
    rows = mixout.shape[0]
    group = n * t
    me = kv * t + tp
    width = group * columns
    offsets = [(o, u) for o in range(n) for u in range(t) if (o, u) != (0, 0)]

    def at(o, u):
        return {"kv": shifted(kv, o, n), "tp": shifted(tp, u, t)}

    def block(o, u):
        return shifted(kv, o, n) * t + shifted(tp, u, t)

    def columns_of(index):
        return pl.ds(pl.multiple_of(index * columns, columns), columns)

    wait_barrier = greet([at(o, u) for o, u in offsets])

    def load(source, target, sem):
        copy = pltpu.make_async_copy(source, target, sem)
        copy.start()
        return copy

    loads_out = [
        load(w_out.at[:, columns_of(shifted(tp, u, t))], out_buf.at[u], load_out.at[u])
        for u in range(t)
    ]
    up_chunks, _, up_width = up_buf.shape
    loads_up = [
        load(w_up.at[:, pl.ds(c * up_width, up_width)], up_buf.at[c], load_up.at[c])
        for c in range(up_chunks)
    ]
    steps = [*range(1, n), 0]
    loads_down = {
        (s, u): load(
            w_down.at[:, columns_of(block(steps[s], u))], down_buf.at[s, u], load_down.at[s, u]
        )
        for s in range(n)
        for u in range(t)
    }
    gathered[kv] = mixout[...]
    affine[me, 0:1] = gain_one[...]
    affine[me, 1:2] = bias_one[...]
    wait_barrier()
    pending = []

    mixes = [
        send(mixout, gathered.at[kv], mix_send.at[o], mix_recv.at[o], at(o, 0))
        for o in range(1, n)
    ]
    affines = [
        send(affine.at[me], affine.at[me], affine_send.at[o, u], affine_recv.at[o, u], at(o, u))
        for o, u in offsets
    ]
    pending += mixes + affines
    for copy in mixes:
        copy.wait_recv()
    whole = gathered[...].reshape(count, gathered.shape[2])
    parts = []
    for u in [*range(1, t), 0]:
        loads_out[u].wait()
        product = jnp.dot(whole, out_buf[u], preferred_element_type=jnp.float32)
        if u:
            part[u - 1] = product
            parts.append(
                send(
                    part.at[u - 1],
                    part_got.at[u - 1],
                    part_send.at[u - 1],
                    part_recv.at[u - 1],
                    at(0, u),
                )
            )
    pending += parts
    own_tokens = tokens[:, columns_of(tp)].astype(jnp.float32)
    first = residual_scale * own_tokens + product
    for u in range(1, t):
        parts[u - 1].wait_recv()
        first = first + part_got[u - 1]
    firsts[me] = first.astype(jnp.bfloat16)

    def pass_on(index, o, u):
        where = at(o, u) if u == 0 else at(0, u)
        copy = send(
            firsts.at[index], firsts.at[index], first_send.at[o, u], first_recv.at[o, u], where
        )
        pending.append(copy)
        return copy

    passed = {}
    for o in range(1, n):
        passed[o, 0] = pass_on(me, o, 0)
    for u in range(1, t):
        passed[0, u] = pass_on(me, 0, u)
    for copy in affines:
        copy.wait_recv()
    for o in range(1, n):
        passed[o, 0].wait_recv()
        for u in range(1, t):
            passed[o, u] = pass_on(block(n - o, 0), o, u)
    for o in range(n):
        for u in range(1, t):
            passed[o, u].wait_recv()

    total = jnp.zeros((count, 1), jnp.float32)
    for g in range(group):
        total = total + jnp.sum(firsts[g].astype(jnp.float32), axis=1, keepdims=True)
    center = total / width
    spread = jnp.zeros((count, 1), jnp.float32)
    for g in range(group):
        away = firsts[g].astype(jnp.float32) - center
        spread = spread + jnp.sum(away * away, axis=1, keepdims=True)
    scale = lax.rsqrt(spread / width + epsilon)

    def finish(values, pair):
        return ((values.astype(jnp.float32) - center) * scale * pair[0:1] + pair[1:2]).astype(
            jnp.bfloat16
        )

    for g in range(group):
        normed[:, g * columns : (g + 1) * columns] = finish(firsts[g], affine[g])
    own_normed = finish(firsts[me], affine[me])

    for c in range(up_chunks):
        loads_up[c].wait()
        upper = jnp.dot(normed[...], up_buf[c], preferred_element_type=jnp.float32)
        upper = jnp.maximum(upper, 0.0)
        hidden[:, c * up_width : (c + 1) * up_width] = (upper * upper).astype(jnp.bfloat16)

    near = {}
    far = {}

    def near_sum(s):
        value = kept[s]
        for u in range(1, t):
            near[s, u].wait_recv()
            value = value + near_got[s, u - 1].astype(jnp.float32)
        return value

    def far_out(s):
        far_sent[s] = near_sum(s).astype(jnp.bfloat16)
        far[s] = send(
            far_sent.at[s], far_got.at[s], far_send.at[s], far_recv.at[s], at(steps[s], 0)
        )

    for s in range(n):
        for u in [*range(1, t), 0]:
            loads_down[s, u].wait()
            product = jnp.dot(hidden[...], down_buf[s, u], preferred_element_type=jnp.float32)
            if u:
                near_sent[s, u - 1] = product.astype(jnp.bfloat16)
                near[s, u] = send(
                    near_sent.at[s, u - 1],
                    near_got.at[s, u - 1],
                    near_send.at[s, u - 1],
                    near_recv.at[s, u - 1],
                    at(0, u),
                )
            else:
                kept[s] = product
        if s:
            far_out(s - 1)
    second = residual_scale * own_normed.astype(jnp.float32) + near_sum(n - 1)
    for s in range(n - 1):
        far[s].wait_recv()
        second = second + far_got[s].astype(jnp.float32)
    pending += list(near.values()) + list(far.values())

    sums = jnp.concatenate(
        [
            to_lanes(jnp.sum(second, axis=1, keepdims=True)),
            to_lanes(jnp.sum(second * second, axis=1, keepdims=True)),
        ],
        axis=0,
    )
    stats[0, 0:2] = sums
    tallies = []
    for i, (o, u) in enumerate(offsets):
        tallies.append(
            send(stats.at[0], stats.at[i + 1], stats_send.at[i], stats_recv.at[i], at(o, u))
        )
    pending += tallies
    for i, copy in enumerate(tallies):
        copy.wait_recv()
        sums = sums + stats[i + 1, 0:2]
    center_two = to_sublanes(sums[0:1]) / width
    spread_two = to_sublanes(sums[1:2]) / width - center_two * center_two
    result = (second - center_two) * lax.rsqrt(spread_two + epsilon) * gain_two[...] + bias_two[...]
    out[...] = result.astype(jnp.bfloat16)
    for copy in pending:
        copy.wait_send()


def mix(mixout, tokens, affine, w_out, w_up, w_down, n, t):
    count = tokens.shape[0]
    rows, heads_width = mixout.shape
    columns = affine[0].shape[1]
    depth, units = w_up.shape
    group = n * t
    up_width = min(units, 512)
    dma = pltpu.SemaphoreType.DMA
    vmem = pltpu.VMEM
    few, many = jnp.bfloat16, jnp.float32
    return pl.pallas_call(
        functools.partial(mix_kernel, n, t),
        out_shape=jax.ShapeDtypeStruct((count, columns), few),
        in_specs=[pl.BlockSpec(memory_space=pltpu.VMEM)] * 6
        + [pl.BlockSpec(memory_space=pl.ANY)] * 3,
        out_specs=pl.BlockSpec(memory_space=pltpu.VMEM),
        scratch_shapes=[
            vmem((t, heads_width, columns), few),
            vmem((units // up_width, depth, up_width), few),
            vmem((n, t, units, columns), few),
            vmem((n, rows, heads_width), few),
            vmem((t - 1, count, columns), many),
            vmem((t - 1, count, columns), many),
            vmem((group, 2, columns), many),
            vmem((group, count, columns), few),
            vmem((count, depth), few),
            vmem((count, units), few),
            vmem((n, t - 1, count, columns), few),
            vmem((n, t - 1, count, columns), few),
            vmem((n, count, columns), many),
            vmem((n, count, columns), few),
            vmem((n, count, columns), few),
            vmem((group, 8, count), many),
            dma((t,)),
            dma((units // up_width,)),
            dma((n, t)),
            dma((n,)),
            dma((n,)),
            dma((t,)),
            dma((t,)),
            dma((n, t)),
            dma((n, t)),
            dma((n, t)),
            dma((n, t)),
            dma((n, t)),
            dma((n, t)),
            dma((n,)),
            dma((n,)),
            dma((group,)),
            dma((group,)),
        ],
        compiler_params=pltpu.CompilerParams(
            collective_id=1, has_side_effects=True, vmem_limit_bytes=VMEM_BYTES
        ),
        name="mix",
    )(mixout, tokens, *affine, w_out, w_up, w_down)


def per_device(
    tokens,
    state,
    w_query,
    w_forget,
    w_input,
    w_gate,
    lower_bound,
    head_gain,
    w_out,
    gain_one,
    bias_one,
    w_up,
    w_down,
    gain_two,
    bias_two,
):
    n, t = lax.axis_size("kv"), lax.axis_size("tp")
    size = head_gain.shape[0]
    heads = w_query.shape[1] // size
    columns, lines = project(
        tokens,
        lower_bound[None, :],
        jnp.tile(head_gain, heads)[None, :],
        (w_query, w_forget, w_input, w_gate),
        n,
        size,
    )
    new_state, mixout = update_state(state, columns, lines)
    result = mix(
        mixout,
        tokens,
        [vector[None, :] for vector in (gain_one, bias_one, gain_two, bias_two)],
        w_out,
        w_up,
        w_down,
        n,
        t,
    )
    return (result, new_state)


def solution(mesh):
    placed = (
        P("dp", "kv"),
        P(("dp", "kv"), "tp", None, None),
        P("kv", "tp"),
        P("kv", "tp"),
        P("kv", "tp"),
        P("kv", "tp"),
        P("tp"),
        P(),
        P("tp", "kv"),
        P(("kv", "tp")),
        P(("kv", "tp")),
        P(None, ("kv", "tp")),
        P(("kv", "tp"), None),
        P(("kv", "tp")),
        P(("kv", "tp")),
    )
    return jax.shard_map(
        per_device,
        mesh=mesh,
        in_specs=placed,
        out_specs=(P("dp", ("kv", "tp")), P(("dp", "kv"), "tp", None, None)),
        check_vma=False,
    )
```

```python
import functools

import jax
import jax.numpy as jnp
import numpy as np
from jax import lax
from jax.experimental import pallas as pl
from jax.experimental.pallas import tpu as pltpu
from jax.sharding import PartitionSpec as P

epsilon = 0.1
residual_scale = 1.68
MESH = pl.DeviceIdType.MESH
VMEM_BYTES = 60 * 1024 * 1024


def shifted(index, by, count):
    return lax.rem(index + by, count)


def greet(peers):
    barrier = pltpu.get_barrier_semaphore()
    for peer in peers:
        pl.semaphore_signal(barrier, inc=1, device_id=peer, device_id_type=MESH)
    return lambda: pl.semaphore_wait(barrier, len(peers))


def send(source, target, send_sem, recv_sem, peer):
    copy = pltpu.make_async_remote_copy(
        src_ref=source,
        dst_ref=target,
        send_sem=send_sem,
        recv_sem=recv_sem,
        device_id=peer,
        device_id_type=MESH,
    )
    copy.start()
    return copy


def project_kernel(
    n,
    chunk,
    size,
    tokens,
    bound,
    wq,
    wf,
    wi,
    wg,
    columns,
    lines,
    wbuf,
    whole,
    sent,
    got,
    load_sem,
    send_sem,
    recv_sem,
):
    me = lax.axis_index("kv")
    weights = (wq, wf, wi, wg)
    per = wq.shape[1] // chunk
    chunks = len(weights) * per
    rows = lines.shape[1]
    peers = [{"kv": shifted(me, o, n)} for o in range(1, n)]
    wait_barrier = greet(peers)
    order = [w * per + j for j in range(per) for w in range(len(weights))]
    loads = {}
    for c in order:
        loads[c] = pltpu.make_async_copy(
            weights[c // per].at[:, pl.ds((c % per) * chunk, chunk)], wbuf.at[c], load_sem.at[c]
        )
        loads[c].start()
    copies = {}
    for c in order:
        loads[c].wait()
        value = jnp.dot(tokens[...], wbuf[c], preferred_element_type=jnp.float32)
        value = value.reshape(n, rows, chunk)
        whole[c] = value
        sent[c] = value.astype(jnp.bfloat16)
        if c == order[0]:
            wait_barrier()
        for o in range(1, n):
            copies[c, o] = send(
                sent.at[c, shifted(me, o, n)],
                got.at[c, o - 1],
                send_sem.at[c, o - 1],
                recv_sem.at[c, o - 1],
                peers[o - 1],
            )

    def summed(c):
        total = whole[c, me]
        for o in range(1, n):
            copies[c, o].wait_recv()
            total = total + got[c, o - 1].astype(jnp.float32)
        return total.astype(jnp.bfloat16).astype(jnp.float32)

    heads = chunk // size
    for j in range(per):
        here = slice(j * chunk, (j + 1) * chunk)
        query_raw, forget_raw, value, gate = (summed(w * per + j) for w in range(len(weights)))
        low = bound[:, here]
        forget = low + (1.0 - low) * jax.nn.sigmoid(forget_raw)
        keyvec = (1.0 - low) * jax.nn.sigmoid(-forget_raw)
        query = query_raw * jax.nn.sigmoid(query_raw)
        for i, factor in enumerate((forget, keyvec, query)):
            high = factor.astype(jnp.bfloat16).astype(jnp.float32)
            stacked = jnp.concatenate([high, factor - high], axis=0)
            turned = stacked.T.reshape(heads, size, 2 * rows).astype(jnp.bfloat16)
            columns[i, j * heads : (j + 1) * heads] = turned
        lines[0, :, here] = value
        lines[1, :, here] = gate * jax.nn.sigmoid(gate)
    for copy in copies.values():
        copy.wait_send()


def project(tokens, bound, weights, n, size):
    count = tokens.shape[0]
    rows = count // n
    depth, width = weights[0].shape
    chunk = min(width, 1024)
    chunks = len(weights) * (width // chunk)
    vmem = pl.BlockSpec(memory_space=pltpu.VMEM)
    return pl.pallas_call(
        functools.partial(project_kernel, n, chunk, size),
        out_shape=(
            jax.ShapeDtypeStruct((3, width // size, size, 2 * rows), jnp.bfloat16),
            jax.ShapeDtypeStruct((2, rows, width), jnp.float32),
        ),
        in_specs=[vmem] * 2 + [pl.BlockSpec(memory_space=pl.ANY)] * len(weights),
        out_specs=(vmem, vmem),
        scratch_shapes=[
            pltpu.VMEM((chunks, depth, chunk), jnp.bfloat16),
            pltpu.VMEM((chunks, n, rows, chunk), jnp.float32),
            pltpu.VMEM((chunks, n, rows, chunk), jnp.bfloat16),
            pltpu.VMEM((chunks, n - 1, rows, chunk), jnp.bfloat16),
            pltpu.SemaphoreType.DMA((chunks,)),
            pltpu.SemaphoreType.DMA((chunks, n - 1)),
            pltpu.SemaphoreType.DMA((chunks, n - 1)),
        ],
        compiler_params=pltpu.CompilerParams(
            collective_id=0, has_side_effects=True, vmem_limit_bytes=VMEM_BYTES
        ),
        name="project",
    )(tokens, bound, *weights)


def state_kernel(state, columns, lines, gain, pick, new_state, mixout, spread, value, read):
    count, heads, size, _ = state.shape
    lanes = pick.shape[1] // count
    factors = columns[...].reshape(3 * heads * size, 2 * count)
    spread[...] = jnp.dot(factors, pick[...], preferred_element_type=jnp.float32)

    def turned(values, h):
        return pltpu.roll(values, (heads - h) * size, 1) if h else values

    for h in range(heads):
        value[h] = turned(lines[0], h)
    gated = []
    for h in range(heads):
        for b in range(count):
            forget, keyvec, query = (
                spread[
                    (i * heads + h) * size : (i * heads + h + 1) * size,
                    b * lanes : b * lanes + size,
                ]
                for i in range(3)
            )
            updated = forget * state[b, h] + keyvec * value[h, b : b + 1, :size]
            new_state[b, h] = updated
            read[h, b : b + 1] = jnp.sum(updated * query, axis=0, keepdims=True)
    for h in range(heads):
        whole = read[h]
        scale = lax.rsqrt(jnp.mean(whole * whole, axis=1, keepdims=True) + epsilon)
        gated.append(whole * scale * gain[...] * turned(lines[1], h)[:, :size])
    mixout[...] = jnp.concatenate(gated, axis=1).astype(jnp.bfloat16)


def update_state(state, columns, lines, gain):
    count, heads, size, _ = state.shape
    lanes = 128
    some = lanes // size
    pick = np.arange(2 * count)[:, None] % count == np.arange(count * lanes) // lanes
    pick = jnp.asarray(pick, jnp.bfloat16)
    return pl.pallas_call(
        state_kernel,
        grid=(heads // some,),
        out_shape=(
            jax.ShapeDtypeStruct(state.shape, jnp.float32),
            jax.ShapeDtypeStruct((count, heads * size), jnp.bfloat16),
        ),
        in_specs=[
            pl.BlockSpec((count, some, size, size), lambda h: (0, h, 0, 0)),
            pl.BlockSpec((3, some, size, 2 * count), lambda h: (0, h, 0, 0)),
            pl.BlockSpec((2, count, lanes), lambda h: (0, 0, h)),
            pl.BlockSpec((1, size), lambda h: (0, 0)),
            pl.BlockSpec((2 * count, count * lanes), lambda h: (0, 0)),
        ],
        out_specs=(
            pl.BlockSpec((count, some, size, size), lambda h: (0, h, 0, 0)),
            pl.BlockSpec((count, lanes), lambda h: (0, h)),
        ),
        scratch_shapes=[
            pltpu.VMEM((3 * some * size, count * lanes), jnp.float32),
            pltpu.VMEM((some, count, lanes), jnp.float32),
            pltpu.VMEM((some, count, size), jnp.float32),
        ],
        compiler_params=pltpu.CompilerParams(vmem_limit_bytes=VMEM_BYTES),
        name="state",
    )(state, columns, lines, gain, pick)


def to_lanes(column):
    count = column.shape[0]
    diagonal = lax.broadcasted_iota(jnp.int32, (count, count), 0) == lax.broadcasted_iota(
        jnp.int32, (count, count), 1
    )
    return jnp.sum(jnp.where(diagonal, column, 0.0), axis=0, keepdims=True)


def to_sublanes(row):
    count = row.shape[1]
    diagonal = lax.broadcasted_iota(jnp.int32, (count, count), 0) == lax.broadcasted_iota(
        jnp.int32, (count, count), 1
    )
    return jnp.sum(jnp.where(diagonal, row, 0.0), axis=1, keepdims=True)


def mix_kernel(
    n,
    t,
    mixout,
    tokens,
    gain_one,
    bias_one,
    gain_two,
    bias_two,
    w_out,
    w_up,
    w_down,
    out,
    out_buf,
    up_buf,
    down_buf,
    gathered,
    part,
    part_got,
    affine,
    firsts,
    normed,
    hidden,
    near_sent,
    near_got,
    kept,
    far_sent,
    far_got,
    stats,
    load_out,
    load_up,
    load_down,
    mix_send,
    mix_recv,
    part_send,
    part_recv,
    affine_send,
    affine_recv,
    first_send,
    first_recv,
    near_send,
    near_recv,
    far_send,
    far_recv,
    stats_send,
    stats_recv,
):
    kv, tp = lax.axis_index("kv"), lax.axis_index("tp")
    count, columns = out.shape
    rows = mixout.shape[0]
    group = n * t
    me = kv * t + tp
    width = group * columns
    offsets = [(o, u) for o in range(n) for u in range(t) if (o, u) != (0, 0)]

    def at(o, u):
        return {"kv": shifted(kv, o, n), "tp": shifted(tp, u, t)}

    def block(o, u):
        return shifted(kv, o, n) * t + shifted(tp, u, t)

    def columns_of(index):
        return pl.ds(pl.multiple_of(index * columns, columns), columns)

    wait_barrier = greet([at(o, u) for o, u in offsets])

    def load(source, target, sem):
        copy = pltpu.make_async_copy(source, target, sem)
        copy.start()
        return copy

    loads_out = [
        load(w_out.at[:, columns_of(shifted(tp, u, t))], out_buf.at[u], load_out.at[u])
        for u in range(t)
    ]
    up_chunks, _, up_width = up_buf.shape
    loads_up = [
        load(w_up.at[:, pl.ds(c * up_width, up_width)], up_buf.at[c], load_up.at[c])
        for c in range(up_chunks)
    ]
    steps = [*range(1, n), 0]
    loads_down = {
        (s, u): load(
            w_down.at[:, columns_of(block(steps[s], u))], down_buf.at[s, u], load_down.at[s, u]
        )
        for s in range(n)
        for u in range(t)
    }
    gathered[kv] = mixout[...]
    affine[me, 0:1] = gain_one[...]
    affine[me, 1:2] = bias_one[...]
    wait_barrier()
    pending = []

    mixes = [
        send(mixout, gathered.at[kv], mix_send.at[o], mix_recv.at[o], at(o, 0))
        for o in range(1, n)
    ]
    affines = [
        send(affine.at[me], affine.at[me], affine_send.at[o, u], affine_recv.at[o, u], at(o, u))
        for o, u in offsets
    ]
    pending += mixes + affines
    for copy in mixes:
        copy.wait_recv()
    whole = gathered[...].reshape(count, gathered.shape[2])
    parts = []
    for u in [*range(1, t), 0]:
        loads_out[u].wait()
        product = jnp.dot(whole, out_buf[u], preferred_element_type=jnp.float32)
        if u:
            part[u - 1] = product
            parts.append(
                send(
                    part.at[u - 1],
                    part_got.at[u - 1],
                    part_send.at[u - 1],
                    part_recv.at[u - 1],
                    at(0, u),
                )
            )
    pending += parts
    own_tokens = tokens[:, columns_of(tp)].astype(jnp.float32)
    first = residual_scale * own_tokens + product
    for u in range(1, t):
        parts[u - 1].wait_recv()
        first = first + part_got[u - 1]
    firsts[me] = first.astype(jnp.bfloat16)

    def pass_on(index, o, u):
        where = at(o, u) if u == 0 else at(0, u)
        copy = send(
            firsts.at[index], firsts.at[index], first_send.at[o, u], first_recv.at[o, u], where
        )
        pending.append(copy)
        return copy

    passed = {}
    for o in range(1, n):
        passed[o, 0] = pass_on(me, o, 0)
    for u in range(1, t):
        passed[0, u] = pass_on(me, 0, u)
    for copy in affines:
        copy.wait_recv()
    for o in range(1, n):
        passed[o, 0].wait_recv()
        for u in range(1, t):
            passed[o, u] = pass_on(block(n - o, 0), o, u)
    for o in range(n):
        for u in range(1, t):
            passed[o, u].wait_recv()

    total = jnp.zeros((count, 1), jnp.float32)
    for g in range(group):
        total = total + jnp.sum(firsts[g].astype(jnp.float32), axis=1, keepdims=True)
    center = total / width
    spread = jnp.zeros((count, 1), jnp.float32)
    for g in range(group):
        away = firsts[g].astype(jnp.float32) - center
        spread = spread + jnp.sum(away * away, axis=1, keepdims=True)
    scale = lax.rsqrt(spread / width + epsilon)

    def finish(values, pair):
        return ((values.astype(jnp.float32) - center) * scale * pair[0:1] + pair[1:2]).astype(
            jnp.bfloat16
        )

    for g in range(group):
        normed[:, g * columns : (g + 1) * columns] = finish(firsts[g], affine[g])
    own_normed = finish(firsts[me], affine[me])

    for c in range(up_chunks):
        loads_up[c].wait()
        upper = jnp.dot(normed[...], up_buf[c], preferred_element_type=jnp.float32)
        upper = jnp.maximum(upper, 0.0)
        hidden[:, c * up_width : (c + 1) * up_width] = (upper * upper).astype(jnp.bfloat16)

    near = {}
    far = {}

    def near_sum(s):
        value = kept[s]
        for u in range(1, t):
            near[s, u].wait_recv()
            value = value + near_got[s, u - 1].astype(jnp.float32)
        return value

    def far_out(s):
        far_sent[s] = near_sum(s).astype(jnp.bfloat16)
        far[s] = send(
            far_sent.at[s], far_got.at[s], far_send.at[s], far_recv.at[s], at(steps[s], 0)
        )

    for s in range(n):
        for u in [*range(1, t), 0]:
            loads_down[s, u].wait()
            product = jnp.dot(hidden[...], down_buf[s, u], preferred_element_type=jnp.float32)
            if u:
                near_sent[s, u - 1] = product.astype(jnp.bfloat16)
                near[s, u] = send(
                    near_sent.at[s, u - 1],
                    near_got.at[s, u - 1],
                    near_send.at[s, u - 1],
                    near_recv.at[s, u - 1],
                    at(0, u),
                )
            else:
                kept[s] = product
        if s:
            far_out(s - 1)
    second = residual_scale * own_normed.astype(jnp.float32) + near_sum(n - 1)
    for s in range(n - 1):
        far[s].wait_recv()
        second = second + far_got[s].astype(jnp.float32)
    pending += list(near.values()) + list(far.values())

    sums = jnp.concatenate(
        [
            to_lanes(jnp.sum(second, axis=1, keepdims=True)),
            to_lanes(jnp.sum(second * second, axis=1, keepdims=True)),
        ],
        axis=0,
    )
    stats[0, 0:2] = sums
    tallies = []
    for i, (o, u) in enumerate(offsets):
        tallies.append(
            send(stats.at[0], stats.at[i + 1], stats_send.at[i], stats_recv.at[i], at(o, u))
        )
    pending += tallies
    for i, copy in enumerate(tallies):
        copy.wait_recv()
        sums = sums + stats[i + 1, 0:2]
    center_two = to_sublanes(sums[0:1]) / width
    spread_two = to_sublanes(sums[1:2]) / width - center_two * center_two
    result = (second - center_two) * lax.rsqrt(spread_two + epsilon) * gain_two[...] + bias_two[...]
    out[...] = result.astype(jnp.bfloat16)
    for copy in pending:
        copy.wait_send()


def mix(mixout, tokens, affine, w_out, w_up, w_down, n, t):
    count = tokens.shape[0]
    rows, heads_width = mixout.shape
    columns = affine[0].shape[1]
    depth, units = w_up.shape
    group = n * t
    up_width = min(units, 512)
    dma = pltpu.SemaphoreType.DMA
    vmem = pltpu.VMEM
    few, many = jnp.bfloat16, jnp.float32
    return pl.pallas_call(
        functools.partial(mix_kernel, n, t),
        out_shape=jax.ShapeDtypeStruct((count, columns), few),
        in_specs=[pl.BlockSpec(memory_space=pltpu.VMEM)] * 6
        + [pl.BlockSpec(memory_space=pl.ANY)] * 3,
        out_specs=pl.BlockSpec(memory_space=pltpu.VMEM),
        scratch_shapes=[
            vmem((t, heads_width, columns), few),
            vmem((units // up_width, depth, up_width), few),
            vmem((n, t, units, columns), few),
            vmem((n, rows, heads_width), few),
            vmem((t - 1, count, columns), many),
            vmem((t - 1, count, columns), many),
            vmem((group, 2, columns), many),
            vmem((group, count, columns), few),
            vmem((count, depth), few),
            vmem((count, units), few),
            vmem((n, t - 1, count, columns), few),
            vmem((n, t - 1, count, columns), few),
            vmem((n, count, columns), many),
            vmem((n, count, columns), few),
            vmem((n, count, columns), few),
            vmem((group, 8, count), many),
            dma((t,)),
            dma((units // up_width,)),
            dma((n, t)),
            dma((n,)),
            dma((n,)),
            dma((t,)),
            dma((t,)),
            dma((n, t)),
            dma((n, t)),
            dma((n, t)),
            dma((n, t)),
            dma((n, t)),
            dma((n, t)),
            dma((n,)),
            dma((n,)),
            dma((group,)),
            dma((group,)),
        ],
        compiler_params=pltpu.CompilerParams(
            collective_id=1, has_side_effects=True, vmem_limit_bytes=VMEM_BYTES
        ),
        name="mix",
    )(mixout, tokens, *affine, w_out, w_up, w_down)


def per_device(
    tokens,
    state,
    w_query,
    w_forget,
    w_input,
    w_gate,
    lower_bound,
    head_gain,
    w_out,
    gain_one,
    bias_one,
    w_up,
    w_down,
    gain_two,
    bias_two,
):
    n, t = lax.axis_size("kv"), lax.axis_size("tp")
    size = head_gain.shape[0]
    columns, lines = project(
        tokens,
        lower_bound[None, :],
        (w_query, w_forget, w_input, w_gate),
        n,
        size,
    )
    new_state, mixout = update_state(state, columns, lines, head_gain[None, :])
    result = mix(
        mixout,
        tokens,
        [vector[None, :] for vector in (gain_one, bias_one, gain_two, bias_two)],
        w_out,
        w_up,
        w_down,
        n,
        t,
    )
    return (result, new_state)


def solution(mesh):
    placed = (
        P("dp", "kv"),
        P(("dp", "kv"), "tp", None, None),
        P("kv", "tp"),
        P("kv", "tp"),
        P("kv", "tp"),
        P("kv", "tp"),
        P("tp"),
        P(),
        P("tp", "kv"),
        P(("kv", "tp")),
        P(("kv", "tp")),
        P(None, ("kv", "tp")),
        P(("kv", "tp"), None),
        P(("kv", "tp")),
        P(("kv", "tp")),
    )
    return jax.shard_map(
        per_device,
        mesh=mesh,
        in_specs=placed,
        out_specs=(P("dp", ("kv", "tp")), P(("dp", "kv"), "tp", None, None)),
        check_vma=False,
    )
```
